1024 devices in a mesh: sp: 16 (over x, core), dp: 64 (over z, y).
Axes of the slice: x: 8, y: 8, z: 8, core: 2. Of those that a mesh axis runs over, the one named last changes fastest.
Arguments:
- queries: bfloat16 [128, 8, 2304, 128], P('dp', None, 'sp'), may hold values from -6 to 6
- keys: bfloat16 [128, 8, 2304, 128], P('dp', None, 'sp'), may hold values from -6 to 6
- values: bfloat16 [128, 8, 2304, 128], P('dp', None, 'sp'), may hold values from -6 to 6
- in_gate: bfloat16 [128, 8, 2304], P('dp', None, 'sp'), may hold values from -5 to 240
- forget_gate: bfloat16 [128, 8, 2304], P('dp', None, 'sp'), may hold values from 1 to 20
- out_gate: bfloat16 [128, 8, 2304, 128], P('dp', None, 'sp'), may hold values from -6 to 6
- norm_gain: float32 [8, 128], replicated, may hold values from 0.1 to 1.9
- out_weight: bfloat16 [1024, 2048], P(None, 'dp'), may hold values from -0.1875 to 0.1875
Outputs:
- mixed: bfloat16 [128, 2304, 2048], P('dp', 'sp')
The draws below stay inside these ranges and needn't reach their ends.
All inputs are finite; a program needn't handle non-finite values.
Results may differ from the reference program's by a relative error of at most 0.0057.
Values may be sent and summed in bfloat16 or wider, within the bound.
A program may use at most 64 MiB of HBM per device.

```python
import jax
import jax.numpy as jnp
from jax import lax

D = 2048
H = 8
DH = 128
BLK = 64
ML_W = 1024
LEN = 2304
SEQS = 128


def draw_in_gate(key, part):
    first, second, third = jax.random.split(jax.random.fold_in(key, 11), 3)
    shape = (SEQS, H, LEN)
    result = jnp.clip(jax.random.normal(first, shape, jnp.float32), -5.0, 5.0)
    return result.astype(jnp.bfloat16)


def draw_forget_gate(key, part):
    first, second, third = jax.random.split(jax.random.fold_in(key, 23), 3)
    shape = (SEQS, H, LEN)
    slow_share = 0.5
    slow = jax.random.bernoulli(first, slow_share, (SEQS, H, 1))
    base = jnp.where(slow, jnp.log(0.6 * LEN), jnp.log(60.0))
    noise = jnp.clip(jax.random.normal(second, shape, jnp.float32) * 0.5, -2.0, 2.0)
    block_factor = jax.random.uniform(third, (SEQS, H, LEN // BLK, 1), jnp.float32, -0.7, 0.7)
    block_factor = jnp.broadcast_to(block_factor, (SEQS, H, LEN // BLK, BLK)).reshape(shape)
    return (base + noise + block_factor).astype(jnp.bfloat16)


def shard_levels(own_key, shape, cuts, least, high):
    level = 1.0
    for axis_at, blocks in cuts:
        steps = jax.random.uniform(jax.random.fold_in(jax.random.fold_in(own_key, 6), axis_at), (blocks,), jnp.float32, least / len(cuts), high / len(cuts))
        level = level * jnp.repeat(jnp.exp(steps), shape[axis_at] // blocks).reshape((-1,) + (1,) * (len(shape) - 1 - axis_at))
    return level


def gaussian(own_key, extent, spread, limit, shards=(), held_as=jnp.bfloat16):
    values = spread * jax.random.normal(own_key, extent, jnp.float32)
    if shards:
        values = values * shard_levels(own_key, extent, shards, -0.22, 0.18)
    return jnp.clip(values, -limit, limit).astype(held_as)


def setup_inputs(seed: int = 0) -> dict:
    key_of = jax.random.split(jax.random.key(seed), 9)
    queries = gaussian(key_of[0], (SEQS, H, LEN, DH), 1.0, 6.0, ((0, 64), (2, 16)))
    keys = gaussian(key_of[1], (SEQS, H, LEN, DH), 1.0, 6.0, ((0, 64), (2, 16)))
    values = gaussian(key_of[2], (SEQS, H, LEN, DH), 1.0, 6.0, ((0, 64), (2, 16)))
    in_gate = draw_in_gate(jax.random.fold_in(key_of[8], 71), 0)
    forget_gate = draw_forget_gate(jax.random.fold_in(key_of[8], 71), 0)
    out_gate = gaussian(key_of[5], (SEQS, H, LEN, DH), 1.0, 6.0, ((0, 64), (2, 16)))
    norm_gain = jnp.clip(1.0 + 0.18 * jax.random.normal(key_of[6], (H, DH), jnp.float32), 0.1, 1.9)
    out_weight = gaussian(key_of[7], (ML_W, D), ML_W ** -0.5, 0.1875, ((1, 64),))
    return dict(queries=queries, keys=keys, values=values, in_gate=in_gate, forget_gate=forget_gate, out_gate=out_gate, norm_gain=norm_gain, out_weight=out_weight)


highest = lax.Precision.HIGHEST
norm_eps = 1e-05

def cell_run(query_in, key_in, value_in, input_in, forget_in):
    head_count = query_in.shape[0]
    head_size = query_in.shape[-1]
    blocks = LEN // BLK

    def to_blocks(array):
        shaped = array.astype(jnp.float32).reshape((head_count, blocks, BLK) + array.shape[2:])
        return jnp.swapaxes(shaped, 0, 1)
    query_b = to_blocks(query_in)
    key_b = to_blocks(key_in) * head_size ** (-0.5)
    value_b = to_blocks(value_in)
    input_b = to_blocks(input_in)
    logf_b = jax.nn.log_sigmoid(to_blocks(forget_in))
    causal_mask = jnp.tril(jnp.ones((BLK, BLK), dtype=bool))

    def advance(state_in, inputs):
        memory, normalizer, stabilizer = state_in
        query_c, key_c, value_c, input_c, logf_c = inputs
        cumulative = jnp.cumsum(logf_c, axis=-1)
        log_weights = cumulative[:, :, None] - cumulative[:, None, :] + input_c[:, None, :]
        log_weights = jnp.where(causal_mask, log_weights, -jnp.inf)
        carried_log = cumulative + stabilizer[:, None]
        row_max = jnp.maximum(lax.optimization_barrier(jnp.max(log_weights, axis=-1)), carried_log)
        w_intra = jnp.exp(log_weights - row_max[:, :, None])
        w_inter = jnp.exp(carried_log - row_max)
        scores = jnp.einsum('hld,hsd->hls', query_c, key_c, precision=highest) * w_intra
        numerator = w_inter[:, :, None] * jnp.einsum('hld,hde->hle', query_c, memory, precision=highest)
        numerator = numerator + jnp.einsum('hls,hse->hle', scores, value_c, precision=highest)
        denominator = w_inter * jnp.einsum('hld,hd->hl', query_c, normalizer, precision=highest) + lax.optimization_barrier(jnp.sum(scores, axis=-1))
        cell_out = numerator / jnp.maximum(jnp.abs(denominator), 1.0)[:, :, None]
        block_end = cumulative[:, -1]
        growth = block_end[:, None] - cumulative + input_c
        stab_new = jnp.maximum(block_end + stabilizer, lax.optimization_barrier(jnp.max(growth, axis=-1)))
        w_key = jnp.exp(growth - stab_new[:, None])
        decay_old = jnp.exp(block_end + stabilizer - stab_new)
        memory = decay_old[:, None, None] * memory + jnp.einsum('hs,hsd,hse->hde', w_key, key_c, value_c, precision=highest)
        normalizer = decay_old[:, None] * normalizer + jnp.einsum('hs,hsd->hd', w_key, key_c, precision=highest)
        return ((memory, normalizer, stab_new), cell_out)
    start = (jnp.zeros((head_count, head_size, head_size), jnp.float32), jnp.zeros((head_count, head_size), jnp.float32), jnp.zeros((head_count,), jnp.float32))
    _, cell_out = lax.scan(advance, start, (query_b, key_b, value_b, input_b, logf_b))
    return jnp.swapaxes(cell_out, 0, 1).reshape(head_count, LEN, head_size).astype(jnp.bfloat16)

def reference(queries, keys, values, in_gate, forget_gate, out_gate, norm_gain, out_weight):

    def per_sequence(packed):
        query_s, key_s, value_s, input_s, forget_s, gate_s = packed
        cell_out = cell_run(query_s, key_s, value_s, input_s, forget_s).astype(jnp.float32)
        mean_val = lax.optimization_barrier(jnp.mean(cell_out, axis=-1, keepdims=True))
        centered = cell_out - mean_val
        variance = lax.optimization_barrier(jnp.mean(centered * centered, axis=-1, keepdims=True))
        normed = centered * lax.rsqrt(variance + norm_eps) * norm_gain[:, None, :]
        hidden = (normed * jax.nn.sigmoid(gate_s.astype(jnp.float32))).astype(jnp.bfloat16)
        flat = jnp.swapaxes(hidden, 0, 1).reshape(LEN, -1)
        return jnp.dot(flat, out_weight, preferred_element_type=jnp.float32).astype(jnp.bfloat16)
    return lax.map(per_sequence, (queries, keys, values, in_gate, forget_gate, out_gate))
```

```python
import functools

import jax
import jax.numpy as jnp
from jax import lax
from jax.experimental import pallas as pl
from jax.experimental.pallas import tpu as pltpu
from jax.sharding import Mesh
from jax.sharding import PartitionSpec as P

MESH = pl.DeviceIdType.MESH
F32 = jnp.float32
BF16 = jnp.bfloat16
HI = lax.Precision.HIGHEST
NT = (((1,), (1,)), ((), ()))
TN = (((0,), (0,)), ((), ()))
EPS = 1e-05
HEADS = 8
PAIRS = 16
T = 144
DH = 128
SROWS = 144
RING = 8
PARTS = ((0, 80), (80, 64))
CUTS = 4
FAR = 2


def kernel(
    q_hbm, k_hbm, v_hbm, ig_hbm, fg_hbm, og_hbm, gain_hbm, w_hbm, o_hbm,
    q_ref, k_ref, v_ref, ig_ref, fg_ref, og_ref, gain_ref, o_ref, in_sem, out_sem,
    wg, state_in, state_out, state_eff, local, peer_local, num_loc, den_loc, top, hid,
    arow, wcol, stat, peer_stat, m_in, m_out, m_eff, coef,
    one_send, one_recv, ring_send, ring_recv, core_w_send, core_w_recv,
    loc_send, loc_recv, ch_send, ch_recv, eff_send, eff_recv, small_send, small_recv,
):
    x = lax.axis_index("x")
    core = lax.axis_index("c")
    z = lax.axis_index("z")
    y = lax.axis_index("y")
    other = {"c": 1 - core}
    barrier = pltpu.get_barrier_semaphore()

    def at(axis, d):
        return {axis: lax.rem(lax.axis_index(axis) + (d + RING), RING)}

    def copy(src, dst, ss, rs, dev):
        return pltpu.make_async_remote_copy(
            src_ref=src, dst_ref=dst, send_sem=ss, recv_sem=rs, device_id=dev, device_id_type=MESH
        )

    def greet(dev):
        pl.semaphore_signal(barrier, inc=1, device_id=dev, device_id_type=MESH)

    greet(other)

    @pl.when(core == 0)
    def _():
        for axis in ("y", "z"):
            for d in range(1, RING):
                greet(at(axis, d))

    @pl.when(core == 1)
    def _():
        greet(at("x", 1))
        greet(at("x", -1))

    loads = [
        pltpu.make_async_copy(src, dst, in_sem.at[i])
        for i, (src, dst) in enumerate(
            (
                (fg_hbm, fg_ref),
                (ig_hbm, ig_ref),
                (k_hbm, k_ref),
                (v_hbm, v_ref),
                (q_hbm, q_ref),
                (og_hbm, og_ref),
                (gain_hbm, gain_ref),
            )
        )
    ]
    w_load = pltpu.make_async_copy(w_hbm, wg.at[z, y], in_sem.at[7])
    for load in loads[:2]:
        load.start()

    @pl.when(core == 0)
    def _():
        w_load.start()

    for load in loads[2:]:
        load.start()

    row_i = lax.broadcasted_iota(jnp.int32, (T, T), 0)
    col_i = lax.broadcasted_iota(jnp.int32, (T, T), 1)
    lower = (col_i <= row_i).astype(BF16)
    eye = (col_i == row_i).astype(BF16)
    loads[0].wait()
    loads[1].wait()
    logf = -jnp.log1p(jnp.exp(-fg_ref[...].astype(F32)))
    rest = logf
    sum_t = jnp.zeros((T, PAIRS), F32)
    sum_r = jnp.zeros((PAIRS, T), F32)
    for _ in range(3):
        term = rest.astype(BF16)
        rest = rest - term.astype(F32)
        sum_t = sum_t + lax.dot_general(lower, term, NT, preferred_element_type=F32)
        sum_r = sum_r + lax.dot_general(term, lower, NT, preferred_element_type=F32)
    inp = ig_ref[...].astype(F32)
    inp_t = lax.dot_general(eye, ig_ref[...], NT, preferred_element_type=F32)
    arow[...] = inp - sum_r
    a_t = inp_t - sum_t
    top_row = jnp.max(a_t, axis=0, keepdims=True)
    w_t = jnp.exp(a_t - top_row) * (DH**-0.5)
    for p in range(PAIRS):
        wcol[p] = jnp.broadcast_to(w_t[:, p : p + 1], (T, DH))
    stat[0:1, 0:PAIRS] = sum_t[T - 1 : T, :]
    stat[1:2, 0:PAIRS] = top_row

    def first(half, d):
        axis = ("y", "z")[half]
        ref = wg.at[z, y, pl.ds(16 * half, 16)]
        return copy(ref, ref, one_send.at[half, d - 1], one_recv.at[half, d - 1], at(axis, d))

    def first_in(half, d):
        axis = ("y", "z")[half]
        n = lax.rem(lax.axis_index(axis) - d + RING, RING)
        dst = wg.at[z, n, pl.ds(0, 16)] if half == 0 else wg.at[n, y, pl.ds(16, 16)]
        return copy(dst, dst, one_send.at[half, d - 1], one_recv.at[half, d - 1], at(axis, d))

    def block(half, n):
        return wg.at[n, :, pl.ds(0, 16)] if half == 0 else wg.at[:, n, pl.ds(16, 16)]

    def half_block(half, n, part):
        cut = pl.ds(4 * part, 4)
        return wg.at[n, cut, pl.ds(0, 16)] if half == 0 else wg.at[cut, n, pl.ds(16, 16)]

    def second_axis(half):
        return ("z", "y")[half]

    def shifted(half, d):
        return lax.rem(lax.axis_index(second_axis(half)) + (d + RING), RING)

    def piece(half, way, s, c):
        cut = pl.ds(c * (RING // CUTS), RING // CUTS)
        n = shifted(half, -way * s)
        return wg.at[n, cut, pl.ds(0, 16)] if half == 0 else wg.at[cut, n, pl.ds(16, 16)]

    def pieces(way, s):
        return range(CUTS) if s < 4 else (range(CUTS // 2), range(CUTS // 2, CUTS))[way < 0]

    def ring_copy(half, way, s, c):
        ref = piece(half, way, s, c)
        f, i = 2 * half + (way < 0), CUTS * s + c
        return copy(ref, ref, ring_send.at[f, i], ring_recv.at[f, i], at(second_axis(half), way))

    def ring_in(half, way, s, c):
        ref = piece(half, way, s, c)
        f, i = 2 * half + (way < 0), CUTS * (s - 1) + c
        return copy(ref, ref, ring_send.at[f, i], ring_recv.at[f, i], at(second_axis(half), way))

    def core_ref(half, slot):
        if slot == 8:
            return block(half, shifted(half, 0))
        way = (1, -1)[slot % 2]
        n = shifted(half, -way * (slot // 2 + 1))
        return block(half, n) if slot < 6 else half_block(half, n, slot - 6)

    def core_copy(half, slot):
        ref = core_ref(half, slot)
        return copy(ref, ref, core_w_send.at[half, slot], core_w_recv.at[half, slot], other)

    stat_copy = copy(stat, peer_stat, small_send.at[0], small_recv.at[0], other)
    m_right = copy(m_out, m_in, small_send.at[1], small_recv.at[1], at("x", 1))
    m_core = copy(m_in, m_eff, small_send.at[2], small_recv.at[2], other)

    def loc_copy(p):
        return copy(local.at[p], peer_local.at[p], loc_send.at[p], loc_recv.at[p], other)

    def chain_copy(p, h):
        rows = pl.ds(*PARTS[h])
        return copy(
            state_out.at[p, rows], state_in.at[p, rows], ch_send.at[p, h], ch_recv.at[p, h], at("x", 1)
        )

    def eff_copy(p, h):
        rows = pl.ds(*PARTS[h])
        return copy(state_in.at[p, rows], state_eff.at[p, rows], eff_send.at[p, h], eff_recv.at[p, h], other)

    @pl.when(x == 0)
    def _():
        zero = jnp.zeros((8, DH), F32)
        m_in[...] = zero

        @pl.when(core == 0)
        def _():
            m_eff[...] = zero

        def clear(p, c):
            state_in[p] = jnp.zeros((SROWS, DH), BF16)

            @pl.when(core == 0)
            def _():
                state_eff[p] = jnp.zeros((SROWS, DH), BF16)

            return c

        lax.fori_loop(0, PAIRS, clear, 0)

    tail_i = lax.broadcasted_iota(jnp.int32, (16, DH), 0)

    def local_state(p, c):
        kw = k_ref[p].astype(F32) * wcol[p]
        n = jnp.sum(kw, axis=0, keepdims=True)
        local[p, 0:DH] = lax.dot_general(v_ref[p], kw.astype(BF16), TN, preferred_element_type=F32)
        local[p, DH:SROWS] = jnp.where(tail_i == 0, jnp.broadcast_to(n, (16, DH)), 0.0)

        return c

    loads[2].wait()
    loads[3].wait()
    lax.fori_loop(0, PAIRS, local_state, 0)

    @pl.when(core == 1)
    def _():
        pl.semaphore_wait(barrier, 3)

    @pl.when(core == 0)
    def _():
        pl.semaphore_wait(barrier, 15)
        stat_copy.start()

        def give(p, c):
            loc_copy(p).start()
            return c

        lax.fori_loop(0, PAIRS, give, 0)
        w_load.wait()
        for d in (4, 3, 5, 2, 6, 1, 7):
            first(0, d).start()
            first(1, d).start()

    for load in loads[4:]:
        load.wait()

    def attend(p, c):
        a = arow[pl.ds(p, 1), :]
        masked = jnp.where(col_i <= row_i, jnp.broadcast_to(a, (T, T)), -1e30)
        t = jnp.max(masked, axis=1, keepdims=True)
        wt = jnp.exp(masked - t) * (DH**-0.5)
        s = lax.dot_general(q_ref[p], k_ref[p], NT, preferred_element_type=F32) * wt
        den_loc[p] = jnp.broadcast_to(jnp.sum(s, axis=1, keepdims=True), (T, DH))
        top[p] = jnp.broadcast_to(t, (T, DH))
        high = s.astype(BF16)
        low = (s - high.astype(F32)).astype(BF16)
        num_loc[p] = jnp.dot(high, v_ref[p], preferred_element_type=F32) + jnp.dot(
            low, v_ref[p], preferred_element_type=F32
        )
        return c

    def attend_all():
        lax.fori_loop(0, PAIRS, attend, 0)

    def finish(p):
        t = top[p]
        m = m_eff_b(p)
        mu = jnp.maximum(t, m)
        g1 = jnp.exp(m - mu)
        g2 = jnp.exp(t - mu)
        inter = lax.dot_general(q_ref[p], state_eff[p], NT, preferred_element_type=F32)
        num = g1 * inter[:, 0:DH] + g2 * num_loc[p]
        den = g1 * jnp.broadcast_to(inter[:, DH : DH + 1], (T, DH)) + g2 * den_loc[p]
        cell = (num / jnp.maximum(jnp.abs(den), 1.0)).astype(BF16).astype(F32)
        mean = jnp.mean(cell, axis=1, keepdims=True)
        cen = cell - mean
        var = jnp.mean(cen * cen, axis=1, keepdims=True)
        h = lax.rem(p, HEADS)
        b = lax.div(p, HEADS)
        gain = gain_ref[pl.ds(h, 1), :]
        gate = 1.0 / (1.0 + jnp.exp(-og_ref[p].astype(F32)))
        out = cen * lax.rsqrt(var + EPS) * gain * gate
        hid[b, :, pl.ds(pl.multiple_of(h * DH, DH), DH)] = out.astype(BF16)

    def m_eff_b(p):
        return coef[4, pl.ds(p, 1), :]

    eye_p = lax.broadcasted_iota(jnp.int32, (PAIRS, PAIRS), 0) == lax.broadcasted_iota(
        jnp.int32, (PAIRS, PAIRS), 1
    )

    def spread(i, row):
        column = jnp.sum(jnp.where(eye_p, jnp.broadcast_to(row, (PAIRS, PAIRS)), 0.0), axis=1, keepdims=True)
        coef[i] = jnp.broadcast_to(column, (PAIRS, DH))

    def chain(p, with_finish):
        loc_copy(p).wait_recv()
        c_old, c_peer = coef[0, pl.ds(p, 1), :], coef[1, pl.ds(p, 1), :]
        c_mid, c_own = coef[2, pl.ds(p, 1), :], coef[3, pl.ds(p, 1), :]
        for h, (row, n) in enumerate(PARTS):
            rows = pl.ds(row, n)
            mid = c_peer * peer_local[p, rows]
            out = c_mid * mid + c_own * local[p, rows]

            @pl.when(x > 0)
            def _():
                chain_copy(p, h).wait_recv()
                eff_copy(p, h).start()

            old = c_old * state_in[p, rows].astype(F32)
            state_out[p, rows] = (c_mid * old + out).astype(BF16)

            @pl.when(x < RING - 1)
            def _():
                chain_copy(p, h).start()

            state_eff[p, rows] = (old + mid).astype(BF16)
        if with_finish:
            finish(p)

    def chain_all(with_finish):
        @pl.when(x > 0)
        def _():
            m_right.wait_recv()

        e0, t0 = peer_stat[0:1, 0:PAIRS], peer_stat[1:2, 0:PAIRS]
        e1, t1 = stat[0:1, 0:PAIRS], stat[1:2, 0:PAIRS]
        m0 = m_in[0:1, 0:PAIRS]
        mu0 = jnp.maximum(m0, t0)
        m1 = e0 + mu0
        mu1 = jnp.maximum(m1, t1)
        m_out[0:1, 0:PAIRS] = e1 + mu1

        @pl.when(x < RING - 1)
        def _():
            m_right.start()

        @pl.when(x > 0)
        def _():
            m_core.start()

        spread(0, jnp.exp(m0 - mu0))
        spread(1, jnp.exp(t0 - mu0))
        spread(2, jnp.exp(m1 - mu1))
        spread(3, jnp.exp(t1 - mu1))
        spread(4, m1)

        def step(p, c):
            chain(p, with_finish)
            return c

        lax.fori_loop(0, PAIRS, step, 0)

    def finish_all():
        def step(p, c):
            finish(p)
            return c

        lax.fori_loop(0, PAIRS, step, 0)

    @pl.when(core == 1)
    def _():
        stat_copy.wait_recv()

        @pl.when(x >= FAR)
        def _():
            attend_all()
            chain_all(True)

        @pl.when(x < FAR)
        def _():
            chain_all(False)
            attend_all()
            finish_all()

        for half in range(2):
            for slot in (8, 0, 1, 2, 3, 4, 5, 6, 7):
                core_copy(half, slot).wait_recv()

    @pl.when(core == 0)
    def _():
        attend_all()
        for half in range(2):
            for d in range(1, RING):
                first_in(half, d).wait_recv()
            for c in range(CUTS):
                for way in (1, -1):
                    ring_copy(half, way, 0, (c, CUTS - 1 - c)[way < 0]).start()
            core_copy(half, 8).start()
        for s in range(1, 5):
            for c in range(CUTS if s < 4 else CUTS // 2):
                for half in range(2):
                    for way in (1, -1):
                        cut = (c, CUTS - 1 - c)[way < 0]
                        ring_in(half, way, s, cut).wait_recv()
                        if s < 4 and cut in pieces(way, s + 1):
                            ring_copy(half, way, s, cut).start()
            for half in range(2):
                core_copy(half, 2 * s - 2).start()
                core_copy(half, 2 * s - 1).start()

        @pl.when(x > 0)
        def _():
            m_core.wait_recv()

        spread(4, m_eff[0:1, 0:PAIRS])

        def step(p, c):
            @pl.when(x > 0)
            def _():
                eff_copy(p, 0).wait_recv()
                eff_copy(p, 1).wait_recv()

            finish(p)
            return c

        lax.fori_loop(0, PAIRS, step, 0)

    def out_copy(i):
        cut = pl.ds(pl.multiple_of(i * 256, 256), 256)
        return pltpu.make_async_copy(o_ref.at[:, :, cut], o_hbm.at[:, :, cut], out_sem.at[i])

    def project(i, c):
        wt = wg[i].reshape(RING * 32, HEADS * DH)
        for b in range(2):
            o_ref[b, :, pl.ds(pl.multiple_of(i * 256, 256), 256)] = lax.dot_general(
                hid[b], wt, NT, preferred_element_type=F32
            ).astype(BF16)
        out_copy(i).start()
        return c

    lax.fori_loop(0, RING, project, 0)

    @pl.when(core == 0)
    def _():
        stat_copy.wait_send()
        for half in range(2):
            for d in range(1, RING):
                first(half, d).wait_send()
            for way in (1, -1):
                for s in range(4):
                    for c in pieces(way, s + 1):
                        ring_copy(half, way, s, c).wait_send()
            for slot in range(9):
                core_copy(half, slot).wait_send()

        def drain(p, c):
            loc_copy(p).wait_send()
            return c

        lax.fori_loop(0, PAIRS, drain, 0)

    @pl.when(core == 1)
    def _():
        @pl.when(x > 0)
        def _():
            m_core.wait_send()

        @pl.when(x < RING - 1)
        def _():
            m_right.wait_send()

        def drain(p, c):
            @pl.when(x > 0)
            def _():
                eff_copy(p, 0).wait_send()
                eff_copy(p, 1).wait_send()

            @pl.when(x < RING - 1)
            def _():
                chain_copy(p, 0).wait_send()
                chain_copy(p, 1).wait_send()

            return c

        lax.fori_loop(0, PAIRS, drain, 0)

    def written(i, c):
        out_copy(i).wait()
        return c

    lax.fori_loop(0, RING, written, 0)


def body(queries, keys, values, in_gate, forget_gate, out_gate, norm_gain, out_weight):
    seqs, heads, span, dh = queries.shape

    def by_pair(a):
        return a.reshape((PAIRS,) + a.shape[2:])

    hbm = pl.BlockSpec(memory_space=pltpu.HBM)
    dma = pltpu.SemaphoreType.DMA
    return pl.pallas_call(
        kernel,
        name="cell",
        out_shape=jax.ShapeDtypeStruct((seqs, span, 2048), BF16),
        in_specs=[hbm] * 8,
        out_specs=hbm,
        scratch_shapes=[
            pltpu.VMEM((PAIRS, T, DH), BF16),
            pltpu.VMEM((PAIRS, T, DH), BF16),
            pltpu.VMEM((PAIRS, T, DH), BF16),
            pltpu.VMEM((PAIRS, T), BF16),
            pltpu.VMEM((PAIRS, T), BF16),
            pltpu.VMEM((PAIRS, T, DH), BF16),
            pltpu.VMEM((HEADS, DH), F32),
            pltpu.VMEM((seqs, span, 2048), BF16),
            dma((8,)),
            dma((8,)),
            pltpu.VMEM((RING, RING, 32, heads * dh), BF16),
            pltpu.VMEM((PAIRS, SROWS, DH), BF16),
            pltpu.VMEM((PAIRS, SROWS, DH), BF16),
            pltpu.VMEM((PAIRS, SROWS, DH), BF16),
            pltpu.VMEM((PAIRS, SROWS, DH), F32),
            pltpu.VMEM((PAIRS, SROWS, DH), F32),
            pltpu.VMEM((PAIRS, T, DH), F32),
            pltpu.VMEM((PAIRS, T, DH), F32),
            pltpu.VMEM((PAIRS, T, DH), F32),
            pltpu.VMEM((2, T, heads * dh), BF16),
            pltpu.VMEM((PAIRS, T), F32),
            pltpu.VMEM((PAIRS, T, DH), F32),
            pltpu.VMEM((8, DH), F32),
            pltpu.VMEM((8, DH), F32),
            pltpu.VMEM((8, DH), F32),
            pltpu.VMEM((8, DH), F32),
            pltpu.VMEM((8, DH), F32),
            pltpu.VMEM((5, PAIRS, DH), F32),
            dma((2, 7)),
            dma((2, 7)),
            dma((4, 4 * CUTS)),
            dma((4, 4 * CUTS)),
            dma((2, 9)),
            dma((2, 9)),
            dma((PAIRS,)),
            dma((PAIRS,)),
            dma((PAIRS, 2)),
            dma((PAIRS, 2)),
            dma((PAIRS, 2)),
            dma((PAIRS, 2)),
            dma((3,)),
            dma((3,)),
        ],
        compiler_params=pltpu.CompilerParams(
            collective_id=0, has_side_effects=True, vmem_limit_bytes=60 * 2**20
        ),
    )(
        by_pair(queries), by_pair(keys), by_pair(values), by_pair(in_gate), by_pair(forget_gate),
        by_pair(out_gate), norm_gain, out_weight.T,
    )


def solution(mesh):
    finer = Mesh(mesh.devices.reshape(8, 2, 8, 8), ("x", "c", "z", "y"))
    sp, dp = ("x", "c"), ("z", "y")
    placed = (
        P(dp, None, sp, None),
        P(dp, None, sp, None),
        P(dp, None, sp, None),
        P(dp, None, sp),
        P(dp, None, sp),
        P(dp, None, sp, None),
        P(),
        P(None, dp),
    )
    return jax.shard_map(
        body, mesh=finer, in_specs=placed, out_specs=P(dp, sp, None), check_vma=False
    )
```

```python
import functools

import jax
import jax.numpy as jnp
from jax import lax
from jax.experimental import pallas as pl
from jax.experimental.pallas import tpu as pltpu
from jax.sharding import Mesh
from jax.sharding import PartitionSpec as P

SC = jax.named_scope
MESH = pl.DeviceIdType.MESH
F32 = jnp.float32
BF16 = jnp.bfloat16
HI = lax.Precision.HIGHEST
NT = (((1,), (1,)), ((), ()))
TN = (((0,), (0,)), ((), ()))
EPS = 1e-05
HEADS = 8
PAIRS = 16
T = 144
DH = 128
SROWS = 144
RING = 8
PARTS = ((0, 80), (80, 64))
CUTS = 4
FAR = 2


def kernel(
    q_hbm, k_hbm, v_hbm, ig_hbm, fg_hbm, og_hbm, gain_hbm, w_hbm, o_ref,
    q_ref, k_ref, v_ref, ig_ref, fg_ref, og_ref, gain_ref, in_sem,
    wg, state_in, state_out, state_eff, local, peer_local, num_loc, den_loc, top, gates, hid,
    arow, wcol, stat, peer_stat, m_in, m_out, m_eff, coef,
    one_send, one_recv, ring_send, ring_recv, core_w_send, core_w_recv,
    loc_send, loc_recv, ch_send, ch_recv, eff_send, eff_recv, small_send, small_recv,
):
    x = lax.axis_index("x")
    core = lax.axis_index("c")
    z = lax.axis_index("z")
    y = lax.axis_index("y")
    other = {"c": 1 - core}
    barrier = pltpu.get_barrier_semaphore()

    def at(axis, d):
        return {axis: lax.rem(lax.axis_index(axis) + (d + RING), RING)}

    def copy(src, dst, ss, rs, dev):
        return pltpu.make_async_remote_copy(
            src_ref=src, dst_ref=dst, send_sem=ss, recv_sem=rs, device_id=dev, device_id_type=MESH
        )

    def drain(ref, sem):
        pltpu.make_async_copy(ref, ref, sem).wait()

    def greet(dev):
        pl.semaphore_signal(barrier, inc=1, device_id=dev, device_id_type=MESH)

    greet(other)

    @pl.when(core == 0)
    def _():
        for axis in ("y", "z"):
            for d in range(1, RING):
                greet(at(axis, d))

    @pl.when(core == 1)
    def _():
        greet(at("x", 1))
        greet(at("x", -1))

    loads = [
        pltpu.make_async_copy(src, dst, in_sem.at[i])
        for i, (src, dst) in enumerate(
            (
                (fg_hbm, fg_ref),
                (ig_hbm, ig_ref),
                (k_hbm, k_ref),
                (v_hbm, v_ref),
                (q_hbm, q_ref),
                (og_hbm, og_ref),
                (gain_hbm, gain_ref),
            )
        )
    ]
    w_load = pltpu.make_async_copy(w_hbm, wg.at[z, y], in_sem.at[7])
    for load in loads[:2]:
        load.start()

    @pl.when(core == 0)
    def _():
        w_load.start()

    for load in loads[2:]:
        load.start()

    row_i = lax.broadcasted_iota(jnp.int32, (T, T), 0)
    col_i = lax.broadcasted_iota(jnp.int32, (T, T), 1)
    lower = (col_i <= row_i).astype(BF16)
    eye = (col_i == row_i).astype(BF16)
    loads[0].wait()
    loads[1].wait()
    logf = -jnp.log1p(jnp.exp(-fg_ref[...].astype(F32)))
    rest = logf
    sum_t = jnp.zeros((T, PAIRS), F32)
    sum_r = jnp.zeros((PAIRS, T), F32)
    for _ in range(3):
        term = rest.astype(BF16)
        rest = rest - term.astype(F32)
        sum_t = sum_t + lax.dot_general(lower, term, NT, preferred_element_type=F32)
        sum_r = sum_r + lax.dot_general(term, lower, NT, preferred_element_type=F32)
    inp = ig_ref[...].astype(F32)
    inp_t = lax.dot_general(eye, ig_ref[...], NT, preferred_element_type=F32)
    arow[...] = inp - sum_r
    a_t = inp_t - sum_t
    top_row = jnp.max(a_t, axis=0, keepdims=True)
    w_t = jnp.exp(a_t - top_row) * (DH**-0.5)
    for p in range(PAIRS):
        wcol[p] = jnp.broadcast_to(w_t[:, p : p + 1], (T, DH))
    stat[0:1, 0:PAIRS] = sum_t[T - 1 : T, :]
    stat[1:2, 0:PAIRS] = top_row

    def first(half, d):
        axis = ("y", "z")[half]
        ref = wg.at[z, y, pl.ds(16 * half, 16)]
        return copy(ref, ref, one_send, one_recv.at[half], at(axis, d))

    def block(half, n):
        return wg.at[n, :, pl.ds(0, 16)] if half == 0 else wg.at[:, n, pl.ds(16, 16)]

    def second_axis(half):
        return ("z", "y")[half]

    def shifted(half, d):
        return lax.rem(lax.axis_index(second_axis(half)) + (d + RING), RING)

    def piece(half, way, s, c):
        cut = pl.ds(c * (RING // CUTS), RING // CUTS)
        n = shifted(half, -way * s)
        return wg.at[n, cut, pl.ds(0, 16)] if half == 0 else wg.at[cut, n, pl.ds(16, 16)]

    def pieces(way, s):
        return range(CUTS) if s < 4 else (range(CUTS // 2), range(CUTS // 2, CUTS))[way < 0]

    def ring_copy(half, way, s, c):
        ref = piece(half, way, s, c)
        f, i = 2 * half + (way < 0), CUTS * s + c
        return copy(ref, ref, ring_send, ring_recv.at[f, i], at(second_axis(half), way))

    def ring_in(half, way, s, c):
        ref = piece(half, way, s, c)
        f, i = 2 * half + (way < 0), CUTS * (s - 1) + c
        return copy(ref, ref, ring_send, ring_recv.at[f, i], at(second_axis(half), way))

    def core_copy(ref):
        return copy(ref, ref, core_w_send, core_w_recv, other)

    stat_copy = copy(stat, peer_stat, small_send.at[0], small_recv.at[0], other)
    m_right = copy(m_out, m_in, small_send.at[1], small_recv.at[1], at("x", 1))
    m_core = copy(m_in, m_eff, small_send.at[2], small_recv.at[2], other)

    def loc_copy(g):
        group = pl.ds(4 * g, 4)
        return copy(local.at[group], peer_local.at[group], loc_send, loc_recv.at[g], other)

    def chain_copy(p, h):
        rows = pl.ds(*PARTS[h])
        return copy(
            state_out.at[p, rows], state_in.at[p, rows], ch_send, ch_recv.at[p, h], at("x", 1)
        )

    def eff_copy(p, h):
        rows = pl.ds(*PARTS[h])
        return copy(state_in.at[p, rows], state_eff.at[p, rows], eff_send, eff_recv.at[lax.div(p, 2)], other)

    @pl.when(x == 0)
    def _():
        zero = jnp.zeros((8, DH), F32)
        m_in[...] = zero

        @pl.when(core == 0)
        def _():
            m_eff[...] = zero

        def clear(p, c):
            state_in[p] = jnp.zeros((SROWS, DH), BF16)

            @pl.when(core == 0)
            def _():
                state_eff[p] = jnp.zeros((SROWS, DH), BF16)

            return c

        lax.fori_loop(0, PAIRS, clear, 0)

    tail_i = lax.broadcasted_iota(jnp.int32, (16, DH), 0)

    def local_state(g, c):
        found = []
        for j in range(4):
            p = 4 * g + j
            kw = k_ref[p].astype(F32) * wcol[p]
            n = jnp.sum(kw, axis=0, keepdims=True)
            memory = lax.dot_general(v_ref[p], kw.astype(BF16), TN, preferred_element_type=F32)
            found.append((p, memory, jnp.where(tail_i == 0, jnp.broadcast_to(n, (16, DH)), 0.0)))
        for p, memory, tail in found:
            local[p, 0:DH] = memory
            local[p, DH:SROWS] = tail
        return c

    with SC("kv_in"):
        loads[2].wait()
        loads[3].wait()
    with SC("local"):
        lax.fori_loop(0, PAIRS // 4, local_state, 0)

    @pl.when(core == 1)
    def _():
        with SC("barrier"):
            pl.semaphore_wait(barrier, 3)

    @pl.when(core == 0)
    def _():
        with SC("barrier"):
            pl.semaphore_wait(barrier, 15)
        stat_copy.start()

        for g in range(4):
            loc_copy(g).start()
        w_load.wait()
        for d in (4, 3, 5, 2, 6, 1, 7):
            first(0, d).start()
            first(1, d).start()

    for load in loads[4:]:
        load.wait()

    def attend(g, c):
        found = []
        for j in range(2):
            p = 2 * g + j
            a = arow[pl.ds(p, 1), :]
            masked = jnp.where(col_i <= row_i, jnp.broadcast_to(a, (T, T)), -1e30)
            t = jnp.max(masked, axis=1, keepdims=True)
            wt = jnp.exp(masked - t) * (DH**-0.5)
            s = lax.dot_general(q_ref[p], k_ref[p], NT, preferred_element_type=F32) * wt
            high = s.astype(BF16)
            low = (s - high.astype(F32)).astype(BF16)
            num = jnp.dot(high, v_ref[p], preferred_element_type=F32) + jnp.dot(
                low, v_ref[p], preferred_element_type=F32
            )
            gate = 0.5 * jnp.tanh(0.5 * og_ref[p].astype(F32)) + 0.5
            gain = gain_ref[pl.ds(lax.rem(2 * g, HEADS) + j, 1), :]
            found.append((p, t, jnp.sum(s, axis=1, keepdims=True), num, gate * gain))
        for p, t, den, num, gate in found:
            gates[p] = gate
            top[p] = jnp.broadcast_to(t, (T, DH))
            den_loc[p] = jnp.broadcast_to(den, (T, DH))
            num_loc[p] = num
        return c

    def attend_all():
        with SC("attend"):
            lax.fori_loop(0, PAIRS // 2, attend, 0)

    def finish(g):
        h = lax.rem(2 * g, HEADS)
        rows = pl.ds(pl.multiple_of(lax.div(2 * g, HEADS) * T, T), T)
        found = []
        for j in range(2):
            p = 2 * g + j
            t = top[p]
            m = m_eff_b(p)
            mu = jnp.maximum(t, m)
            g1 = jnp.exp(m - mu)
            g2 = jnp.exp(t - mu)
            inter = lax.dot_general(q_ref[p], state_eff[p], NT, preferred_element_type=F32)
            num = g1 * inter[:, 0:DH] + g2 * num_loc[p]
            den = g1 * jnp.broadcast_to(inter[:, DH : DH + 1], (T, DH)) + g2 * den_loc[p]
            cell = (num / jnp.maximum(jnp.abs(den), 1.0)).astype(BF16).astype(F32)
            mean = jnp.mean(cell, axis=1, keepdims=True)
            cen = cell - mean
            var = jnp.mean(cen * cen, axis=1, keepdims=True)
            found.append((cen * lax.rsqrt(var + EPS) * gates[p]).astype(BF16))
        hid[rows, pl.ds(pl.multiple_of(h * DH, 2 * DH), 2 * DH)] = jnp.concatenate(found, axis=1)

    def m_eff_b(p):
        return coef[4, pl.ds(p, 1), :]

    eye_p = lax.broadcasted_iota(jnp.int32, (PAIRS, PAIRS), 0) == lax.broadcasted_iota(
        jnp.int32, (PAIRS, PAIRS), 1
    )

    def spread(i, row):
        column = jnp.sum(jnp.where(eye_p, jnp.broadcast_to(row, (PAIRS, PAIRS)), 0.0), axis=1, keepdims=True)
        coef[i] = jnp.broadcast_to(column, (PAIRS, DH))

    def chain(p):
        c_old, c_peer = coef[0, pl.ds(p, 1), :], coef[1, pl.ds(p, 1), :]
        c_mid, c_own = coef[2, pl.ds(p, 1), :], coef[3, pl.ds(p, 1), :]
        for h, (row, n) in enumerate(PARTS):
            rows = pl.ds(row, n)
            mid = c_peer * peer_local[p, rows]
            out = c_mid * mid + c_own * local[p, rows]

            @pl.when(x > 0)
            def _():
                with SC("ch_wait"):
                    chain_copy(p, h).wait_recv()
                eff_copy(p, h).start()

            old = c_old * state_in[p, rows].astype(F32)
            state_out[p, rows] = (c_mid * old + out).astype(BF16)

            @pl.when(x < RING - 1)
            def _():
                chain_copy(p, h).start()

            state_eff[p, rows] = (old + mid).astype(BF16)

    def chain_all(with_finish):
        @pl.when(x > 0)
        def _():
            with SC("m_right"):
                m_right.wait_recv()

        e0, t0 = peer_stat[0:1, 0:PAIRS], peer_stat[1:2, 0:PAIRS]
        e1, t1 = stat[0:1, 0:PAIRS], stat[1:2, 0:PAIRS]
        m0 = m_in[0:1, 0:PAIRS]
        mu0 = jnp.maximum(m0, t0)
        m1 = e0 + mu0
        mu1 = jnp.maximum(m1, t1)
        m_out[0:1, 0:PAIRS] = e1 + mu1

        @pl.when(x < RING - 1)
        def _():
            m_right.start()

        @pl.when(x > 0)
        def _():
            m_core.start()

        spread(0, jnp.exp(m0 - mu0))
        spread(1, jnp.exp(t0 - mu0))
        spread(2, jnp.exp(m1 - mu1))
        spread(3, jnp.exp(t1 - mu1))
        spread(4, m1)

        def step(g, c):
            loc_copy(g).wait_recv()
            for j in range(2):
                chain(4 * g + 2 * j)
                chain(4 * g + 2 * j + 1)
                if with_finish:
                    finish(2 * g + j)
            return c

        lax.fori_loop(0, PAIRS // 4, step, 0)

    def finish_all():
        def step(g, c):
            finish(g)
            return c

        with SC("finish"):
            lax.fori_loop(0, PAIRS // 2, step, 0)

    @pl.when(core == 1)
    def _():
        with SC("stat"):
            stat_copy.wait_recv()

        @pl.when(x >= FAR)
        def _():
            attend_all()
            chain_all(True)

        @pl.when(x < FAR)
        def _():
            chain_all(False)
            attend_all()
            finish_all()

        with SC("w_wait"):
            drain(wg, core_w_recv)

    @pl.when(core == 0)
    def _():
        attend_all()
        for half in range(2):
            with SC("first"):
                drain(wg.at[pl.ds(0, RING - 1), 0, pl.ds(0, 16)], one_recv.at[half])
            for c in range(CUTS):
                for way in (1, -1):
                    ring_copy(half, way, 0, (c, CUTS - 1 - c)[way < 0]).start()
            core_copy(block(half, shifted(half, 0))).start()
        for s in range(1, 5):
            with SC("ring"):
                for c in range(CUTS if s < 4 else CUTS // 2):
                    for half in range(2):
                        for way in (1, -1):
                            cut = (c, CUTS - 1 - c)[way < 0]
                            ring_in(half, way, s, cut).wait_recv()
                            if s < 4 and cut in pieces(way, s + 1):
                                ring_copy(half, way, s, cut).start()
                            core_copy(piece(half, way, s, cut)).start()

        @pl.when(x > 0)
        def _():
            m_core.wait_recv()

        spread(4, m_eff[0:1, 0:PAIRS])

        def step(g, c):
            @pl.when(x > 0)
            def _():
                with SC("eff_wait"):
                    drain(state_eff.at[pl.ds(2 * g, 2)], eff_recv.at[g])

            finish(g)
            return c

        lax.fori_loop(0, PAIRS // 2, step, 0)

    def project(i, c):
        for j in range(2):
            n = 2 * i + j
            wt = wg[n].reshape(RING * 32, HEADS * DH)
            cut = pl.ds(pl.multiple_of(n * 256, 256), 256)
            res = lax.dot_general(hid[...], wt, NT, preferred_element_type=F32).astype(BF16)
            o_ref[0, :, cut] = res[0:T]
            o_ref[1, :, cut] = res[T:]
        return c

    with SC("project"):
        lax.fori_loop(0, RING // 2, project, 0)

    @pl.when(core == 0)
    def _():
        stat_copy.wait_send()
        drain(local, loc_send)
        drain(wg.at[pl.ds(0, RING - 1), pl.ds(0, 2), pl.ds(0, 16)], one_send)
        drain(wg.at[pl.ds(0, RING - 1)], ring_send)
        drain(wg, core_w_send)

    @pl.when(core == 1)
    def _():
        @pl.when(x > 0)
        def _():
            m_core.wait_send()
            drain(state_in, eff_send)

        @pl.when(x < RING - 1)
        def _():
            m_right.wait_send()
            drain(state_out, ch_send)


def body(queries, keys, values, in_gate, forget_gate, out_gate, norm_gain, out_weight):
    seqs, heads, span, dh = queries.shape

    def by_pair(a):
        return a.reshape((PAIRS,) + a.shape[2:])

    hbm = pl.BlockSpec(memory_space=pltpu.HBM)
    dma = pltpu.SemaphoreType.DMA
    return pl.pallas_call(
        kernel,
        name="cell",
        out_shape=pltpu.VMEM((seqs, span, 2048), BF16),
        in_specs=[hbm] * 8,
        out_specs=pl.BlockSpec(memory_space=pltpu.VMEM),
        scratch_shapes=[
            pltpu.VMEM((PAIRS, T, DH), BF16),
            pltpu.VMEM((PAIRS, T, DH), BF16),
            pltpu.VMEM((PAIRS, T, DH), BF16),
            pltpu.VMEM((PAIRS, T), BF16),
            pltpu.VMEM((PAIRS, T), BF16),
            pltpu.VMEM((PAIRS, T, DH), BF16),
            pltpu.VMEM((HEADS, DH), F32),
            dma((8,)),
            pltpu.VMEM((RING, RING, 32, heads * dh), BF16),
            pltpu.VMEM((PAIRS, SROWS, DH), BF16),
            pltpu.VMEM((PAIRS, SROWS, DH), BF16),
            pltpu.VMEM((PAIRS, SROWS, DH), BF16),
            pltpu.VMEM((PAIRS, SROWS, DH), F32),
            pltpu.VMEM((PAIRS, SROWS, DH), F32),
            pltpu.VMEM((PAIRS, T, DH), F32),
            pltpu.VMEM((PAIRS, T, DH), F32),
            pltpu.VMEM((PAIRS, T, DH), F32),
            pltpu.VMEM((PAIRS, T, DH), F32),
            pltpu.VMEM((2 * T, heads * dh), BF16),
            pltpu.VMEM((PAIRS, T), F32),
            pltpu.VMEM((PAIRS, T, DH), F32),
            pltpu.VMEM((8, DH), F32),
            pltpu.VMEM((8, DH), F32),
            pltpu.VMEM((8, DH), F32),
            pltpu.VMEM((8, DH), F32),
            pltpu.VMEM((8, DH), F32),
            pltpu.VMEM((5, PAIRS, DH), F32),
            dma,
            dma((2,)),
            dma,
            dma((4, 4 * CUTS)),
            dma,
            dma,
            dma,
            dma((4,)),
            dma,
            dma((PAIRS, 2)),
            dma,
            dma((PAIRS // 2,)),
            dma((3,)),
            dma((3,)),
        ],
        compiler_params=pltpu.CompilerParams(
            collective_id=0, has_side_effects=True, vmem_limit_bytes=60 * 2**20
        ),
    )(
        by_pair(queries), by_pair(keys), by_pair(values), by_pair(in_gate), by_pair(forget_gate),
        by_pair(out_gate), norm_gain, out_weight.T,
    )


def solution(mesh):
    finer = Mesh(mesh.devices.reshape(8, 2, 8, 8), ("x", "c", "z", "y"))
    sp, dp = ("x", "c"), ("z", "y")
    placed = (
        P(dp, None, sp, None),
        P(dp, None, sp, None),
        P(dp, None, sp, None),
        P(dp, None, sp),
        P(dp, None, sp),
        P(dp, None, sp, None),
        P(),
        P(None, dp),
    )
    return jax.shard_map(
        body, mesh=finer, in_specs=placed, out_specs=P(dp, sp, None), check_vma=False
    )
```

```python
import functools

import jax
import jax.numpy as jnp
from jax import lax
from jax.experimental import pallas as pl
from jax.experimental.pallas import tpu as pltpu
from jax.sharding import Mesh
from jax.sharding import PartitionSpec as P

SC = jax.named_scope
MESH = pl.DeviceIdType.MESH
F32 = jnp.float32
BF16 = jnp.bfloat16
HI = lax.Precision.HIGHEST
NT = (((1,), (1,)), ((), ()))
TN = (((0,), (0,)), ((), ()))
EPS = 1e-05
HEADS = 8
PAIRS = 16
T = 144
DH = 128
SROWS = 144
RING = 8
PARTS = ((0, 64), (64, 64))
CUTS = 4
FAR = 2


def kernel(
    q_hbm, k_hbm, v_hbm, ig_hbm, fg_hbm, og_hbm, gain_hbm, w_hbm, o_ref,
    q_ref, k_ref, v_ref, ig_ref, fg_ref, og_ref, gain_ref, in_sem,
    wg, state_in, state_out, state_eff, local, peer_local, num_loc, den_loc, top, gates, hid,
    arow, wcol, stat, peer_stat, m_in, m_out, m_eff, n_in, n_out, n_eff, coef,
    one_send, one_recv, ring_send, ring_recv, core_w_send, core_w_recv,
    loc_send, loc_recv, ch_send, ch_recv, eff_send, eff_recv, small_send, small_recv,
):
    x = lax.axis_index("x")
    core = lax.axis_index("c")
    z = lax.axis_index("z")
    y = lax.axis_index("y")
    other = {"c": 1 - core}
    barrier = pltpu.get_barrier_semaphore()

    def at(axis, d):
        return {axis: lax.rem(lax.axis_index(axis) + (d + RING), RING)}

    def copy(src, dst, ss, rs, dev):
        return pltpu.make_async_remote_copy(
            src_ref=src, dst_ref=dst, send_sem=ss, recv_sem=rs, device_id=dev, device_id_type=MESH
        )

    def drain(ref, sem):
        pltpu.make_async_copy(ref, ref, sem).wait()

    def greet(dev):
        pl.semaphore_signal(barrier, inc=1, device_id=dev, device_id_type=MESH)

    greet(other)

    @pl.when(core == 0)
    def _():
        for axis in ("y", "z"):
            for d in range(1, RING):
                greet(at(axis, d))

    @pl.when(core == 1)
    def _():
        greet(at("x", 1))
        greet(at("x", -1))

    loads = [
        pltpu.make_async_copy(src, dst, in_sem.at[i])
        for i, (src, dst) in enumerate(
            (
                (fg_hbm, fg_ref),
                (ig_hbm, ig_ref),
                (k_hbm, k_ref),
                (v_hbm, v_ref),
                (q_hbm, q_ref),
                (og_hbm, og_ref),
                (gain_hbm, gain_ref),
            )
        )
    ]
    w_load = pltpu.make_async_copy(w_hbm, wg.at[z, y], in_sem.at[7])
    for load in loads[:2]:
        load.start()

    @pl.when(core == 0)
    def _():
        w_load.start()

    for load in loads[2:]:
        load.start()

    row_i = lax.broadcasted_iota(jnp.int32, (T, T), 0)
    col_i = lax.broadcasted_iota(jnp.int32, (T, T), 1)
    lower = (col_i <= row_i).astype(BF16)
    eye = (col_i == row_i).astype(BF16)
    loads[0].wait()
    loads[1].wait()
    logf = -jnp.log1p(jnp.exp(-fg_ref[...].astype(F32)))
    rest = logf
    sum_t = jnp.zeros((T, PAIRS), F32)
    sum_r = jnp.zeros((PAIRS, T), F32)
    for _ in range(3):
        term = rest.astype(BF16)
        rest = rest - term.astype(F32)
        sum_t = sum_t + lax.dot_general(lower, term, NT, preferred_element_type=F32)
        sum_r = sum_r + lax.dot_general(term, lower, NT, preferred_element_type=F32)
    inp = ig_ref[...].astype(F32)
    inp_t = lax.dot_general(eye, ig_ref[...], NT, preferred_element_type=F32)
    arow[...] = inp - sum_r
    a_t = inp_t - sum_t
    top_row = jnp.max(a_t, axis=0, keepdims=True)
    w_t = jnp.exp(a_t - top_row) * (DH**-0.5)
    for p in range(PAIRS):
        wcol[p] = jnp.broadcast_to(w_t[:, p : p + 1], (T, DH))
    stat[0:1, 0:PAIRS] = sum_t[T - 1 : T, :]
    stat[1:2, 0:PAIRS] = top_row

    def first(half, d):
        axis = ("y", "z")[half]
        ref = wg.at[z, y, pl.ds(16 * half, 16)]
        return copy(ref, ref, one_send, one_recv.at[half], at(axis, d))

    def block(half, n):
        return wg.at[n, :, pl.ds(0, 16)] if half == 0 else wg.at[:, n, pl.ds(16, 16)]

    def second_axis(half):
        return ("z", "y")[half]

    def shifted(half, d):
        return lax.rem(lax.axis_index(second_axis(half)) + (d + RING), RING)

    def piece(half, way, s, c):
        cut = pl.ds(c * (RING // CUTS), RING // CUTS)
        n = shifted(half, -way * s)
        return wg.at[n, cut, pl.ds(0, 16)] if half == 0 else wg.at[cut, n, pl.ds(16, 16)]

    def pieces(way, s):
        return range(CUTS) if s < 4 else (range(CUTS // 2), range(CUTS // 2, CUTS))[way < 0]

    def ring_copy(half, way, s, c):
        ref = piece(half, way, s, c)
        f, i = 2 * half + (way < 0), CUTS * s + (c if s < 3 else c % 2)
        return copy(ref, ref, ring_send, ring_recv.at[f, i], at(second_axis(half), way))

    def ring_in(half, way, s, c):
        ref = piece(half, way, s, c)
        f, i = 2 * half + (way < 0), CUTS * (s - 1) + (c if s < 4 else c % 2)
        return copy(ref, ref, ring_send, ring_recv.at[f, i], at(second_axis(half), way))

    def core_copy(ref):
        return copy(ref, ref, core_w_send, core_w_recv, other)

    stat_copy = copy(stat, peer_stat, small_send.at[0], small_recv.at[0], other)
    m_right = copy(m_out, m_in, small_send.at[1], small_recv.at[1], at("x", 1))
    m_core = copy(m_in, m_eff, small_send.at[2], small_recv.at[2], other)
    n_right = copy(n_out, n_in, small_send.at[3], small_recv.at[3], at("x", 1))
    n_core = copy(n_in, n_eff, small_send.at[4], small_recv.at[4], other)

    def loc_copy(g):
        group = pl.ds(4 * g, 4)
        return copy(local.at[group], peer_local.at[group], loc_send, loc_recv.at[g], other)

    def chain_copy(p, h):
        rows = pl.ds(*PARTS[h])
        return copy(
            state_out.at[p, rows], state_in.at[p, rows], ch_send, ch_recv.at[p, h], at("x", 1)
        )

    def eff_copy(p, h):
        rows = pl.ds(*PARTS[h])
        return copy(state_in.at[p, rows], state_eff.at[p, rows], eff_send, eff_recv.at[lax.div(p, 2)], other)

    @pl.when(x == 0)
    def _():
        zero = jnp.zeros((8, DH), F32)
        m_in[...] = zero
        n_in[...] = jnp.zeros((PAIRS, DH), F32)

        @pl.when(core == 0)
        def _():
            m_eff[...] = zero
            n_eff[...] = jnp.zeros((PAIRS, DH), F32)

        def clear(p, c):
            state_in[p] = jnp.zeros((DH, DH), BF16)

            @pl.when(core == 0)
            def _():
                state_eff[p, 0:DH] = jnp.zeros((DH, DH), BF16)

            return c

        lax.fori_loop(0, PAIRS, clear, 0)

    tail_i = lax.broadcasted_iota(jnp.int32, (16, DH), 0)

    def local_state(g, c):
        found = []
        for j in range(4):
            p = 4 * g + j
            kw = k_ref[p].astype(F32) * wcol[p]
            n = jnp.sum(kw, axis=0, keepdims=True)
            memory = lax.dot_general(v_ref[p], kw.astype(BF16), TN, preferred_element_type=F32)
            found.append((p, memory, n))
        for p, memory, n in found:
            local[p] = memory
            stat[pl.ds(8 + p, 1), :] = n
        return c

    with SC("kv_in"):
        loads[2].wait()
        loads[3].wait()
    with SC("local"):
        lax.fori_loop(0, PAIRS // 4, local_state, 0)

    @pl.when(core == 1)
    def _():
        with SC("barrier"):
            pl.semaphore_wait(barrier, 3)

    @pl.when(core == 0)
    def _():
        with SC("barrier"):
            pl.semaphore_wait(barrier, 15)
        stat_copy.start()

        for g in range(4):
            loc_copy(g).start()
        w_load.wait()
        for d in (4, 3, 5, 2, 6, 1, 7):
            first(0, d).start()
            first(1, d).start()

    for load in loads[4:]:
        load.wait()

    def attend(g, c):
        found = []
        for j in range(2):
            p = 2 * g + j
            a = arow[pl.ds(p, 1), :]
            masked = jnp.where(col_i <= row_i, jnp.broadcast_to(a, (T, T)), -1e30)
            t = jnp.max(masked, axis=1, keepdims=True)
            wt = jnp.exp(masked - t) * (DH**-0.5)
            s = lax.dot_general(q_ref[p], k_ref[p], NT, preferred_element_type=F32) * wt
            high = s.astype(BF16)
            low = (s - high.astype(F32)).astype(BF16)
            num = jnp.dot(high, v_ref[p], preferred_element_type=F32) + jnp.dot(
                low, v_ref[p], preferred_element_type=F32
            )
            gate = 0.5 * jnp.tanh(0.5 * og_ref[p].astype(F32)) + 0.5
            gain = gain_ref[pl.ds(lax.rem(2 * g, HEADS) + j, 1), :]
            found.append((p, t, jnp.sum(s, axis=1, keepdims=True), num, gate * gain))
        for p, t, den, num, gate in found:
            gates[p] = gate
            top[p] = jnp.broadcast_to(t, (T, DH))
            den_loc[p] = jnp.broadcast_to(den, (T, DH))
            num_loc[p] = num
        return c

    def attend_all():
        with SC("attend"):
            lax.fori_loop(0, PAIRS // 2, attend, 0)

    def finish(begin, count):
        h = lax.rem(begin, HEADS)
        rows = pl.ds(pl.multiple_of(lax.div(begin, HEADS) * T, T), T)
        found = []
        for j in range(count):
            p = begin + j
            t = top[p]
            m = m_eff_b(p)
            mu = jnp.maximum(t, m)
            g1 = jnp.exp(m - mu)
            g2 = jnp.exp(t - mu)
            inter = lax.dot_general(q_ref[p], state_eff[p], NT, preferred_element_type=F32)
            num = g1 * inter[:, 0:DH] + g2 * num_loc[p]
            den = g1 * jnp.broadcast_to(inter[:, DH : DH + 1], (T, DH)) + g2 * den_loc[p]
            cell = (num / jnp.maximum(jnp.abs(den), 1.0)).astype(BF16).astype(F32)
            mean = jnp.mean(cell, axis=1, keepdims=True)
            cen = cell - mean
            var = jnp.mean(cen * cen, axis=1, keepdims=True)
            found.append((cen * lax.rsqrt(var + EPS) * gates[p]).astype(BF16))
        cut = pl.ds(pl.multiple_of(h * DH, count * DH), count * DH)
        hid[rows, cut] = jnp.concatenate(found, axis=1)

    def m_eff_b(p):
        return coef[4, pl.ds(p, 1), :]

    eye_p = lax.broadcasted_iota(jnp.int32, (PAIRS, PAIRS), 0) == lax.broadcasted_iota(
        jnp.int32, (PAIRS, PAIRS), 1
    )

    def spread(i, row):
        column = jnp.sum(jnp.where(eye_p, jnp.broadcast_to(row, (PAIRS, PAIRS)), 0.0), axis=1, keepdims=True)
        coef[i] = jnp.broadcast_to(column, (PAIRS, DH))

    def chain(p):
        c_old, c_peer = coef[0, pl.ds(p, 1), :], coef[1, pl.ds(p, 1), :]
        c_mid, c_own = coef[2, pl.ds(p, 1), :], coef[3, pl.ds(p, 1), :]
        for h, (row, n) in enumerate(PARTS):
            rows = pl.ds(row, n)
            mid = c_peer * peer_local[p, rows]
            out = c_mid * mid + c_own * local[p, rows]

            @pl.when(x > 0)
            def _():
                with SC("ch_wait"):
                    chain_copy(p, h).wait_recv()
                eff_copy(p, h).start()

            old = c_old * state_in[p, rows].astype(F32)
            state_out[p, rows] = (c_mid * old + out).astype(BF16)

            @pl.when(x < RING - 1)
            def _():
                chain_copy(p, h).start()

            state_eff[p, rows] = (old + mid).astype(BF16)

    def fill_tails():
        def step(p, c):
            n = jnp.broadcast_to(n_eff[pl.ds(p, 1), :], (16, DH))
            state_eff[p, DH:SROWS] = jnp.where(tail_i == 0, n, 0.0).astype(BF16)
            return c

        lax.fori_loop(0, PAIRS, step, 0)

    def chain_all(with_finish):
        @pl.when(x > 0)
        def _():
            with SC("m_right"):
                m_right.wait_recv()

        e0, t0 = peer_stat[0:1, 0:PAIRS], peer_stat[1:2, 0:PAIRS]
        e1, t1 = stat[0:1, 0:PAIRS], stat[1:2, 0:PAIRS]
        m0 = m_in[0:1, 0:PAIRS]
        mu0 = jnp.maximum(m0, t0)
        m1 = e0 + mu0
        mu1 = jnp.maximum(m1, t1)
        m_out[0:1, 0:PAIRS] = e1 + mu1

        @pl.when(x < RING - 1)
        def _():
            m_right.start()

        @pl.when(x > 0)
        def _():
            m_core.start()

        spread(0, jnp.exp(m0 - mu0))
        spread(1, jnp.exp(t0 - mu0))
        spread(2, jnp.exp(m1 - mu1))
        spread(3, jnp.exp(t1 - mu1))
        spread(4, m1)

        @pl.when(x > 0)
        def _():
            n_right.wait_recv()
            n_core.start()

        n_mid = coef[0] * n_in[...] + coef[1] * peer_stat[8:24, :]
        n_out[...] = coef[2] * n_mid + coef[3] * stat[8:24, :]
        n_eff[...] = n_mid

        @pl.when(x < RING - 1)
        def _():
            n_right.start()

        fill_tails()

        def step(g, c):
            loc_copy(g).wait_recv()
            for j in range(2):
                chain(4 * g + 2 * j)
                chain(4 * g + 2 * j + 1)
                if with_finish:
                    finish(4 * g + 2 * j, 2)
            return c

        lax.fori_loop(0, PAIRS // 4, step, 0)

    def finish_all():
        def step(g, c):
            finish(4 * g, 4)
            return c

        with SC("finish"):
            lax.fori_loop(0, PAIRS // 4, step, 0)

    @pl.when(core == 1)
    def _():
        with SC("stat"):
            stat_copy.wait_recv()

        @pl.when(x >= FAR)
        def _():
            attend_all()
            chain_all(True)

        @pl.when(x < FAR)
        def _():
            chain_all(False)
            attend_all()
            finish_all()

        with SC("w_wait"):
            drain(wg, core_w_recv)

    @pl.when(core == 0)
    def _():
        attend_all()
        for half in range(2):
            with SC("first"):
                drain(wg.at[pl.ds(0, RING - 1), 0, pl.ds(0, 16)], one_recv.at[half])
            for c in range(CUTS):
                for way in (1, -1):
                    ring_copy(half, way, 0, (c, CUTS - 1 - c)[way < 0]).start()
            core_copy(block(half, shifted(half, 0))).start()
        for s in range(1, 5):
            with SC("ring"):
                for c in range(CUTS if s < 4 else CUTS // 2):
                    for half in range(2):
                        for way in (1, -1):
                            cut = (c, CUTS - 1 - c)[way < 0]
                            ring_in(half, way, s, cut).wait_recv()
                            if s < 4 and cut in pieces(way, s + 1):
                                ring_copy(half, way, s, cut).start()
                            core_copy(piece(half, way, s, cut)).start()

        @pl.when(x > 0)
        def _():
            m_core.wait_recv()

        spread(4, m_eff[0:1, 0:PAIRS])

        @pl.when(x > 0)
        def _():
            n_core.wait_recv()

        fill_tails()

        def arrived(g):
            @pl.when(x > 0)
            def _():
                with SC("eff_wait"):
                    drain(state_in.at[pl.ds(2 * g, 2)], eff_recv.at[g])

        def step(g, c):
            arrived(2 * g)
            arrived(2 * g + 1)
            finish(4 * g, 4)
            return c

        lax.fori_loop(0, PAIRS // 4 - 1, step, 0)
        for g in (PAIRS // 2 - 2, PAIRS // 2 - 1):
            arrived(g)
            finish(2 * g, 2)

    def project(i, c):
        for j in range(2):
            n = 2 * i + j
            wt = wg[n].reshape(RING * 32, HEADS * DH)
            cut = pl.ds(pl.multiple_of(n * 256, 256), 256)
            res = lax.dot_general(hid[...], wt, NT, preferred_element_type=F32).astype(BF16)
            o_ref[0, :, cut] = res[0:T]
            o_ref[1, :, cut] = res[T:]
        return c

    with SC("project"):
        lax.fori_loop(0, RING // 2, project, 0)

    @pl.when(core == 0)
    def _():
        stat_copy.wait_send()
        drain(local, loc_send)
        drain(wg.at[pl.ds(0, RING - 1), pl.ds(0, 2), pl.ds(0, 16)], one_send)
        drain(wg.at[pl.ds(0, RING - 1)], ring_send)
        drain(wg, core_w_send)

    @pl.when(core == 1)
    def _():
        @pl.when(x > 0)
        def _():
            m_core.wait_send()
            n_core.wait_send()
            drain(state_in, eff_send)

        @pl.when(x < RING - 1)
        def _():
            m_right.wait_send()
            n_right.wait_send()
            drain(state_out, ch_send)


def body(queries, keys, values, in_gate, forget_gate, out_gate, norm_gain, out_weight):
    seqs, heads, span, dh = queries.shape

    def by_pair(a):
        return a.reshape((PAIRS,) + a.shape[2:])

    hbm = pl.BlockSpec(memory_space=pltpu.HBM)
    dma = pltpu.SemaphoreType.DMA
    return pl.pallas_call(
        kernel,
        name="cell",
        out_shape=pltpu.VMEM((seqs, span, 2048), BF16),
        in_specs=[hbm] * 8,
        out_specs=pl.BlockSpec(memory_space=pltpu.VMEM),
        scratch_shapes=[
            pltpu.VMEM((PAIRS, T, DH), BF16),
            pltpu.VMEM((PAIRS, T, DH), BF16),
            pltpu.VMEM((PAIRS, T, DH), BF16),
            pltpu.VMEM((PAIRS, T), BF16),
            pltpu.VMEM((PAIRS, T), BF16),
            pltpu.VMEM((PAIRS, T, DH), BF16),
            pltpu.VMEM((HEADS, DH), F32),
            dma((8,)),
            pltpu.VMEM((RING, RING, 32, heads * dh), BF16),
            pltpu.VMEM((PAIRS, DH, DH), BF16),
            pltpu.VMEM((PAIRS, DH, DH), BF16),
            pltpu.VMEM((PAIRS, SROWS, DH), BF16),
            pltpu.VMEM((PAIRS, DH, DH), F32),
            pltpu.VMEM((PAIRS, DH, DH), F32),
            pltpu.VMEM((PAIRS, T, DH), F32),
            pltpu.VMEM((PAIRS, T, DH), F32),
            pltpu.VMEM((PAIRS, T, DH), F32),
            pltpu.VMEM((PAIRS, T, DH), F32),
            pltpu.VMEM((2 * T, heads * dh), BF16),
            pltpu.VMEM((PAIRS, T), F32),
            pltpu.VMEM((PAIRS, T, DH), F32),
            pltpu.VMEM((24, DH), F32),
            pltpu.VMEM((24, DH), F32),
            pltpu.VMEM((8, DH), F32),
            pltpu.VMEM((8, DH), F32),
            pltpu.VMEM((8, DH), F32),
            pltpu.VMEM((PAIRS, DH), F32),
            pltpu.VMEM((PAIRS, DH), F32),
            pltpu.VMEM((PAIRS, DH), F32),
            pltpu.VMEM((5, PAIRS, DH), F32),
            dma,
            dma((2,)),
            dma,
            dma((4, 3 * CUTS + CUTS // 2)),
            dma,
            dma,
            dma,
            dma((4,)),
            dma,
            dma((PAIRS, 2)),
            dma,
            dma((PAIRS // 2,)),
            dma((5,)),
            dma((5,)),
        ],
        compiler_params=pltpu.CompilerParams(
            collective_id=0, has_side_effects=True, vmem_limit_bytes=60 * 2**20
        ),
    )(
        by_pair(queries), by_pair(keys), by_pair(values), by_pair(in_gate), by_pair(forget_gate),
        by_pair(out_gate), norm_gain, out_weight.T,
    )


def solution(mesh):
    finer = Mesh(mesh.devices.reshape(8, 2, 8, 8), ("x", "c", "z", "y"))
    sp, dp = ("x", "c"), ("z", "y")
    placed = (
        P(dp, None, sp, None),
        P(dp, None, sp, None),
        P(dp, None, sp, None),
        P(dp, None, sp),
        P(dp, None, sp),
        P(dp, None, sp, None),
        P(),
        P(None, dp),
    )
    return jax.shard_map(
        body, mesh=finer, in_specs=placed, out_specs=P(dp, sp, None), check_vma=False
    )
```

```python
import functools

import jax
import jax.numpy as jnp
from jax import lax
from jax.experimental import pallas as pl
from jax.experimental.pallas import tpu as pltpu
from jax.sharding import Mesh
from jax.sharding import PartitionSpec as P

SC = jax.named_scope
MESH = pl.DeviceIdType.MESH
F32 = jnp.float32
BF16 = jnp.bfloat16
HI = lax.Precision.HIGHEST
NT = (((1,), (1,)), ((), ()))
TN = (((0,), (0,)), ((), ()))
EPS = 1e-05
HEADS = 8
PAIRS = 16
T = 144
DH = 128
SROWS = 144
RING = 8
PARTS = ((0, 64), (64, 64))
CUTS = 4
FAR = 2


def kernel(
    q_hbm, k_hbm, v_hbm, ig_hbm, fg_hbm, og_hbm, gain_hbm, w_hbm, o_ref,
    q_ref, k_ref, v_ref, ig_ref, fg_ref, og_ref, gain_ref, in_sem,
    wg, state_in, state_out, state_eff, local, peer_local, num_loc, den_loc, top, gates, hid,
    arow, wcol, stat, peer_stat, m_in, m_out, m_eff, n_in, n_out, n_eff, coef,
    one_send, one_recv, ring_send, ring_recv, core_w_send, core_w_recv,
    loc_send, loc_recv, ch_send, ch_recv, eff_send, eff_recv, small_send, small_recv,
):
    x = lax.axis_index("x")
    core = lax.axis_index("c")
    z = lax.axis_index("z")
    y = lax.axis_index("y")
    other = {"c": 1 - core}
    barrier = pltpu.get_barrier_semaphore()

    def at(axis, d):
        return {axis: lax.rem(lax.axis_index(axis) + (d + RING), RING)}

    def copy(src, dst, ss, rs, dev):
        return pltpu.make_async_remote_copy(
            src_ref=src, dst_ref=dst, send_sem=ss, recv_sem=rs, device_id=dev, device_id_type=MESH
        )

    def drain(ref, sem):
        pltpu.make_async_copy(ref, ref, sem).wait()

    def greet(dev):
        pl.semaphore_signal(barrier, inc=1, device_id=dev, device_id_type=MESH)

    greet(other)

    @pl.when(core == 0)
    def _():
        for axis in ("y", "z"):
            for d in range(1, RING):
                greet(at(axis, d))

    @pl.when(core == 1)
    def _():
        greet(at("x", 1))
        greet(at("x", -1))

    loads = [
        pltpu.make_async_copy(src, dst, in_sem.at[i])
        for i, (src, dst) in enumerate(
            (
                (fg_hbm, fg_ref),
                (ig_hbm, ig_ref),
                (k_hbm, k_ref),
                (v_hbm, v_ref),
                (q_hbm, q_ref),
                (og_hbm, og_ref),
                (gain_hbm, gain_ref),
            )
        )
    ]
    w_load = pltpu.make_async_copy(w_hbm, wg.at[z, y], in_sem.at[7])
    for load in loads[:2]:
        load.start()

    @pl.when(core == 0)
    def _():
        w_load.start()

    for load in loads[2:]:
        load.start()

    row_i = lax.broadcasted_iota(jnp.int32, (T, T), 0)
    col_i = lax.broadcasted_iota(jnp.int32, (T, T), 1)
    lower = (col_i <= row_i).astype(BF16)
    eye = (col_i == row_i).astype(BF16)
    loads[0].wait()
    loads[1].wait()
    logf = -jnp.log1p(jnp.exp(-fg_ref[...].astype(F32)))
    rest = logf
    sum_t = jnp.zeros((T, PAIRS), F32)
    sum_r = jnp.zeros((PAIRS, T), F32)
    for _ in range(3):
        term = rest.astype(BF16)
        rest = rest - term.astype(F32)
        sum_t = sum_t + lax.dot_general(lower, term, NT, preferred_element_type=F32)
        sum_r = sum_r + lax.dot_general(term, lower, NT, preferred_element_type=F32)
    inp = ig_ref[...].astype(F32)
    inp_t = lax.dot_general(eye, ig_ref[...], NT, preferred_element_type=F32)
    arow[...] = inp - sum_r
    a_t = inp_t - sum_t
    top_row = jnp.max(a_t, axis=0, keepdims=True)
    w_t = jnp.exp(a_t - top_row) * (DH**-0.5)
    for p in range(PAIRS):
        wcol[p] = jnp.broadcast_to(w_t[:, p : p + 1], (T, DH))
    stat[0:1, 0:PAIRS] = sum_t[T - 1 : T, :]
    stat[1:2, 0:PAIRS] = top_row

    def first(half, d):
        axis = ("y", "z")[half]
        ref = wg.at[z, y, pl.ds(16 * half, 16)]
        return copy(ref, ref, one_send, one_recv.at[half], at(axis, d))

    def block(half, n):
        return wg.at[n, :, pl.ds(0, 16)] if half == 0 else wg.at[:, n, pl.ds(16, 16)]

    def second_axis(half):
        return ("z", "y")[half]

    def shifted(half, d):
        return lax.rem(lax.axis_index(second_axis(half)) + (d + RING), RING)

    def piece(half, way, s, c):
        cut = pl.ds(c * (RING // CUTS), RING // CUTS)
        n = shifted(half, -way * s)
        return wg.at[n, cut, pl.ds(0, 16)] if half == 0 else wg.at[cut, n, pl.ds(16, 16)]

    def pieces(way, s):
        return range(CUTS) if s < 4 else (range(CUTS // 2), range(CUTS // 2, CUTS))[way < 0]

    def ring_copy(half, way, s, c):
        ref = piece(half, way, s, c)
        f, i = 2 * half + (way < 0), CUTS * s + (c if s < 3 else c % 2)
        return copy(ref, ref, ring_send, ring_recv.at[f, i], at(second_axis(half), way))

    def ring_in(half, way, s, c):
        ref = piece(half, way, s, c)
        f, i = 2 * half + (way < 0), CUTS * (s - 1) + (c if s < 4 else c % 2)
        return copy(ref, ref, ring_send, ring_recv.at[f, i], at(second_axis(half), way))

    def core_copy(ref):
        return copy(ref, ref, core_w_send, core_w_recv, other)

    stat_copy = copy(stat, peer_stat, small_send.at[0], small_recv.at[0], other)
    m_right = copy(m_out, m_in, small_send.at[1], small_recv.at[1], at("x", 1))
    m_core = copy(m_in, m_eff, small_send.at[2], small_recv.at[2], other)
    n_right = copy(n_out, n_in, small_send.at[3], small_recv.at[3], at("x", 1))
    n_core = copy(n_in, n_eff, small_send.at[4], small_recv.at[4], other)

    def loc_copy(g):
        group = pl.ds(4 * g, 4)
        return copy(local.at[group], peer_local.at[group], loc_send, loc_recv.at[g], other)

    def chain_copy(p, h):
        rows = pl.ds(*PARTS[h])
        return copy(
            state_out.at[p, rows], state_in.at[p, rows], ch_send, ch_recv.at[p, h], at("x", 1)
        )

    def eff_copy(p, h):
        rows = pl.ds(*PARTS[h])
        return copy(state_in.at[p, rows], state_eff.at[p, rows], eff_send, eff_recv.at[lax.div(p, 2)], other)

    @pl.when(x == 0)
    def _():
        zero = jnp.zeros((8, DH), F32)
        m_in[...] = zero
        n_in[...] = jnp.zeros((PAIRS, DH), F32)

        @pl.when(core == 0)
        def _():
            m_eff[...] = zero
            n_eff[...] = jnp.zeros((PAIRS, DH), F32)

        def clear(p, c):
            state_in[p] = jnp.zeros((DH, DH), BF16)

            @pl.when(core == 0)
            def _():
                state_eff[p, 0:DH] = jnp.zeros((DH, DH), BF16)

            return c

        lax.fori_loop(0, PAIRS, clear, 0)

    tail_i = lax.broadcasted_iota(jnp.int32, (16, DH), 0)

    def local_state(g, c):
        found = []
        for j in range(4):
            p = 4 * g + j
            kw = k_ref[p].astype(F32) * wcol[p]
            n = jnp.sum(kw, axis=0, keepdims=True)
            memory = lax.dot_general(v_ref[p], kw.astype(BF16), TN, preferred_element_type=F32)
            found.append((p, memory, n))
        for p, memory, n in found:
            local[p] = memory
            stat[pl.ds(8 + p, 1), :] = n
        return c

    with SC("kv_in"):
        loads[2].wait()
        loads[3].wait()
    with SC("local"):
        lax.fori_loop(0, PAIRS // 4, local_state, 0)

    @pl.when(core == 1)
    def _():
        with SC("barrier"):
            pl.semaphore_wait(barrier, 3)

    @pl.when(core == 0)
    def _():
        with SC("barrier"):
            pl.semaphore_wait(barrier, 15)
        stat_copy.start()

        for g in range(4):
            loc_copy(g).start()
        w_load.wait()
        for d in (4, 3, 5, 2, 6, 1, 7):
            first(0, d).start()
            first(1, d).start()

    for load in loads[4:]:
        load.wait()

    def attend(g, c):
        found = []
        for j in range(2):
            p = 2 * g + j
            a = arow[pl.ds(p, 1), :]
            masked = jnp.where(col_i <= row_i, jnp.broadcast_to(a, (T, T)), -1e30)
            t = jnp.max(masked, axis=1, keepdims=True)
            wt = jnp.exp(masked - t) * (DH**-0.5)
            s = lax.dot_general(q_ref[p], k_ref[p], NT, preferred_element_type=F32) * wt
            high = s.astype(BF16)
            low = (s - high.astype(F32)).astype(BF16)
            num = jnp.dot(high, v_ref[p], preferred_element_type=F32) + jnp.dot(
                low, v_ref[p], preferred_element_type=F32
            )
            gate = 0.5 * jnp.tanh(0.5 * og_ref[p].astype(F32)) + 0.5
            gain = gain_ref[pl.ds(lax.rem(2 * g, HEADS) + j, 1), :]
            found.append((p, t, jnp.sum(s, axis=1, keepdims=True), num, gate * gain))
        for p, t, den, num, gate in found:
            gates[p] = gate
            top[p] = jnp.broadcast_to(t, (T, DH))
            den_loc[p] = jnp.broadcast_to(den, (T, DH))
            num_loc[p] = num
        return c

    def attend_all():
        with SC("attend"):
            lax.fori_loop(0, PAIRS // 2, attend, 0)

    def finish(begin, count):
        h = lax.rem(begin, HEADS)
        rows = pl.ds(pl.multiple_of(lax.div(begin, HEADS) * T, T), T)
        found = []
        for j in range(count):
            p = begin + j
            t = top[p]
            m = m_eff_b(p)
            mu = jnp.maximum(t, m)
            g1 = jnp.exp(m - mu)
            g2 = jnp.exp(t - mu)
            inter = lax.dot_general(q_ref[p], state_eff[p], NT, preferred_element_type=F32)
            num = g1 * inter[:, 0:DH] + g2 * num_loc[p]
            den = g1 * jnp.broadcast_to(inter[:, DH : DH + 1], (T, DH)) + g2 * den_loc[p]
            cell = (num / jnp.maximum(jnp.abs(den), 1.0)).astype(BF16).astype(F32)
            mean = jnp.mean(cell, axis=1, keepdims=True)
            cen = cell - mean
            var = jnp.mean(cen * cen, axis=1, keepdims=True)
            found.append((cen * lax.rsqrt(var + EPS) * gates[p]).astype(BF16))
        cut = pl.ds(pl.multiple_of(h * DH, count * DH), count * DH)
        hid[rows, cut] = jnp.concatenate(found, axis=1)

    def m_eff_b(p):
        return coef[4, pl.ds(p, 1), :]

    eye_p = lax.broadcasted_iota(jnp.int32, (PAIRS, PAIRS), 0) == lax.broadcasted_iota(
        jnp.int32, (PAIRS, PAIRS), 1
    )

    def spread(i, row):
        column = jnp.sum(jnp.where(eye_p, jnp.broadcast_to(row, (PAIRS, PAIRS)), 0.0), axis=1, keepdims=True)
        coef[i] = jnp.broadcast_to(column, (PAIRS, DH))

    def chain(p):
        c_old, c_peer = coef[0, pl.ds(p, 1), :], coef[1, pl.ds(p, 1), :]
        c_mid, c_own = coef[2, pl.ds(p, 1), :], coef[3, pl.ds(p, 1), :]
        for h, (row, n) in enumerate(PARTS):
            rows = pl.ds(row, n)
            mid = c_peer * peer_local[p, rows]
            out = c_mid * mid + c_own * local[p, rows]

            @pl.when(x > 0)
            def _():
                with SC("ch_wait"):
                    chain_copy(p, h).wait_recv()
                eff_copy(p, h).start()

            old = c_old * state_in[p, rows].astype(F32)
            state_out[p, rows] = (c_mid * old + out).astype(BF16)

            @pl.when(x < RING - 1)
            def _():
                chain_copy(p, h).start()

            state_eff[p, rows] = (old + mid).astype(BF16)

    def fill_tails():
        def step(p, c):
            n = jnp.broadcast_to(n_eff[pl.ds(p, 1), :], (16, DH))
            state_eff[p, DH:SROWS] = jnp.where(tail_i == 0, n, 0.0).astype(BF16)
            return c

        lax.fori_loop(0, PAIRS, step, 0)

    def chain_all(with_finish):
        @pl.when(x > 0)
        def _():
            with SC("m_right"):
                m_right.wait_recv()

        e0, t0 = peer_stat[0:1, 0:PAIRS], peer_stat[1:2, 0:PAIRS]
        e1, t1 = stat[0:1, 0:PAIRS], stat[1:2, 0:PAIRS]
        m0 = m_in[0:1, 0:PAIRS]
        mu0 = jnp.maximum(m0, t0)
        m1 = e0 + mu0
        mu1 = jnp.maximum(m1, t1)
        m_out[0:1, 0:PAIRS] = e1 + mu1

        @pl.when(x < RING - 1)
        def _():
            m_right.start()

        @pl.when(x > 0)
        def _():
            m_core.start()

        spread(0, jnp.exp(m0 - mu0))
        spread(1, jnp.exp(t0 - mu0))
        spread(2, jnp.exp(m1 - mu1))
        spread(3, jnp.exp(t1 - mu1))
        spread(4, m1)

        @pl.when(x > 0)
        def _():
            n_right.wait_recv()
            n_core.start()

        n_mid = coef[0] * n_in[...] + coef[1] * peer_stat[8:24, :]
        n_out[...] = coef[2] * n_mid + coef[3] * stat[8:24, :]
        n_eff[...] = n_mid

        @pl.when(x < RING - 1)
        def _():
            n_right.start()

        fill_tails()

        def step(g, c):
            loc_copy(g).wait_recv()
            for j in range(2):
                chain(4 * g + 2 * j)
                chain(4 * g + 2 * j + 1)
                if with_finish:
                    finish(4 * g + 2 * j, 2)
            return c

        lax.fori_loop(0, PAIRS // 4, step, 0)

    def finish_all():
        def step(g, c):
            finish(4 * g, 4)
            return c

        with SC("finish"):
            lax.fori_loop(0, PAIRS // 4, step, 0)

    @pl.when(core == 1)
    def _():
        with SC("stat"):
            stat_copy.wait_recv()

        @pl.when(x >= FAR)
        def _():
            attend_all()
            chain_all(True)

        @pl.when(x < FAR)
        def _():
            chain_all(False)
            attend_all()
            finish_all()

        with SC("w_wait"):
            drain(wg, core_w_recv)

    @pl.when(core == 0)
    def _():
        attend_all()
        for half in range(2):
            with SC("first"):
                drain(wg.at[pl.ds(0, RING - 1), 0, pl.ds(0, 16)], one_recv.at[half])
            for c in range(CUTS):
                for way in (1, -1):
                    ring_copy(half, way, 0, (c, CUTS - 1 - c)[way < 0]).start()
            core_copy(block(half, shifted(half, 0))).start()
        for s in range(1, 5):
            with SC("ring"):
                for c in range(CUTS if s < 4 else CUTS // 2):
                    for half in range(2):
                        for way in (1, -1):
                            cut = (c, CUTS - 1 - c)[way < 0]
                            ring_in(half, way, s, cut).wait_recv()
                            if s < 4 and cut in pieces(way, s + 1):
                                ring_copy(half, way, s, cut).start()
                            core_copy(piece(half, way, s, cut)).start()

        @pl.when(x > 0)
        def _():
            m_core.wait_recv()

        spread(4, m_eff[0:1, 0:PAIRS])

        @pl.when(x > 0)
        def _():
            n_core.wait_recv()

        fill_tails()

        def arrived(g):
            @pl.when(x > 0)
            def _():
                with SC("eff_wait"):
                    drain(state_in.at[pl.ds(2 * g, 2)], eff_recv.at[g])

        def step(g, c):
            arrived(2 * g)
            arrived(2 * g + 1)
            finish(4 * g, 4)
            return c

        lax.fori_loop(0, PAIRS // 4 - 1, step, 0)
        for g in (PAIRS // 2 - 2, PAIRS // 2 - 1):
            arrived(g)
            finish(2 * g, 2)

    def project(i, c):
        for j in range(4):
            n = 4 * i + j
            wt = wg[n].reshape(RING * 32, HEADS * DH)
            cut = pl.ds(pl.multiple_of(n * 256, 256), 256)
            res = lax.dot_general(hid[...], wt, NT, preferred_element_type=F32).astype(BF16)
            o_ref[0, :, cut] = res[0:T]
            o_ref[1, :, cut] = res[T:]
        return c

    with SC("project"):
        lax.fori_loop(0, RING // 4, project, 0)

    @pl.when(core == 0)
    def _():
        stat_copy.wait_send()
        drain(local, loc_send)
        drain(wg.at[pl.ds(0, RING - 1), pl.ds(0, 2), pl.ds(0, 16)], one_send)
        drain(wg.at[pl.ds(0, RING - 1)], ring_send)
        drain(wg, core_w_send)

    @pl.when(core == 1)
    def _():
        @pl.when(x > 0)
        def _():
            m_core.wait_send()
            n_core.wait_send()
            drain(state_in, eff_send)

        @pl.when(x < RING - 1)
        def _():
            m_right.wait_send()
            n_right.wait_send()
            drain(state_out, ch_send)


def body(queries, keys, values, in_gate, forget_gate, out_gate, norm_gain, out_weight):
    seqs, heads, span, dh = queries.shape

    def by_pair(a):
        return a.reshape((PAIRS,) + a.shape[2:])

    hbm = pl.BlockSpec(memory_space=pltpu.HBM)
    dma = pltpu.SemaphoreType.DMA
    return pl.pallas_call(
        kernel,
        name="cell",
        out_shape=pltpu.VMEM((seqs, span, 2048), BF16),
        in_specs=[hbm] * 8,
        out_specs=pl.BlockSpec(memory_space=pltpu.VMEM),
        scratch_shapes=[
            pltpu.VMEM((PAIRS, T, DH), BF16),
            pltpu.VMEM((PAIRS, T, DH), BF16),
            pltpu.VMEM((PAIRS, T, DH), BF16),
            pltpu.VMEM((PAIRS, T), BF16),
            pltpu.VMEM((PAIRS, T), BF16),
            pltpu.VMEM((PAIRS, T, DH), BF16),
            pltpu.VMEM((HEADS, DH), F32),
            dma((8,)),
            pltpu.VMEM((RING, RING, 32, heads * dh), BF16),
            pltpu.VMEM((PAIRS, DH, DH), BF16),
            pltpu.VMEM((PAIRS, DH, DH), BF16),
            pltpu.VMEM((PAIRS, SROWS, DH), BF16),
            pltpu.VMEM((PAIRS, DH, DH), F32),
            pltpu.VMEM((PAIRS, DH, DH), F32),
            pltpu.VMEM((PAIRS, T, DH), F32),
            pltpu.VMEM((PAIRS, T, DH), F32),
            pltpu.VMEM((PAIRS, T, DH), F32),
            pltpu.VMEM((PAIRS, T, DH), F32),
            pltpu.VMEM((2 * T, heads * dh), BF16),
            pltpu.VMEM((PAIRS, T), F32),
            pltpu.VMEM((PAIRS, T, DH), F32),
            pltpu.VMEM((24, DH), F32),
            pltpu.VMEM((24, DH), F32),
            pltpu.VMEM((8, DH), F32),
            pltpu.VMEM((8, DH), F32),
            pltpu.VMEM((8, DH), F32),
            pltpu.VMEM((PAIRS, DH), F32),
            pltpu.VMEM((PAIRS, DH), F32),
            pltpu.VMEM((PAIRS, DH), F32),
            pltpu.VMEM((5, PAIRS, DH), F32),
            dma,
            dma((2,)),
            dma,
            dma((4, 3 * CUTS + CUTS // 2)),
            dma,
            dma,
            dma,
            dma((4,)),
            dma,
            dma((PAIRS, 2)),
            dma,
            dma((PAIRS // 2,)),
            dma((5,)),
            dma((5,)),
        ],
        compiler_params=pltpu.CompilerParams(
            collective_id=0, has_side_effects=True, vmem_limit_bytes=60 * 2**20
        ),
    )(
        by_pair(queries), by_pair(keys), by_pair(values), by_pair(in_gate), by_pair(forget_gate),
        by_pair(out_gate), norm_gain, out_weight.T,
    )


def solution(mesh):
    finer = Mesh(mesh.devices.reshape(8, 2, 8, 8), ("x", "c", "z", "y"))
    sp, dp = ("x", "c"), ("z", "y")
    placed = (
        P(dp, None, sp, None),
        P(dp, None, sp, None),
        P(dp, None, sp, None),
        P(dp, None, sp),
        P(dp, None, sp),
        P(dp, None, sp, None),
        P(),
        P(None, dp),
    )
    return jax.shard_map(
        body, mesh=finer, in_specs=placed, out_specs=P(dp, sp, None), check_vma=False
    )
```
